32 devices in a mesh: gr: 2 (over x), fs: 8 (over z, y), tp: 2 (over core).
Axes of the slice: x: 2, y: 2, z: 4, core: 2. Of those that a mesh axis runs over, the one named last changes fastest.
Arguments:
- tokens: bfloat16 [4096, 2048], P(('gr', 'fs')), may hold values from -6 to 6
- norm_gain: float32 [2048], P(('gr', 'fs')), may hold values from 0.1 to 1.9
- gate_train: float32 [8, 2048, 1024], P(None, ('gr', 'fs'), 'tp'), may hold values from -0.125 to 0.125
- up_train: float32 [8, 2048, 1024], P(None, ('gr', 'fs'), 'tp'), may hold values from -0.125 to 0.125
- down_train: float32 [8, 1024, 2048], P(None, 'tp', ('gr', 'fs')), may hold values from -0.1875 to 0.1875
- expert_ids: int32 [4096, 2], P(('gr', 'fs')), may hold values from 0 to 7, all different within a row; in each aligned block of 256 rows (0 to 255, 256 to 511, ...) at most 128 rows name the same one
- route_score: float32 [4096, 2], P(('gr', 'fs')), may hold values from 0.05 to 1
Outputs:
- gate_ready: bfloat16 [8, 2048, 1024], P('fs', None, 'tp')
- up_ready: bfloat16 [8, 2048, 1024], P('fs', None, 'tp')
- down_ready: bfloat16 [8, 1024, 2048], P('fs', 'tp')
- mixed: bfloat16 [4096, 2048], P(('gr', 'fs'), 'tp')
The draws below stay inside these ranges and needn't reach their ends.
Inputs may be any that keep to these rules, and one draw needn't show every extreme that they name: `expert_ids`: each row names two different experts. Among the 256 rows of one device no expert is named more than 128 times, and in every draw some expert is named exactly 128 times by some device's rows.
All inputs are finite; a program needn't handle non-finite values.
Results may differ from the reference program's by a relative error of at most 0.015.
Values may be sent and summed in bfloat16 or wider, within the bound.
No kernel may reach another device: no remote copies, remote signals or barrier semaphores. Data moves between devices by JAX's collectives and lax.ppermute only.
A program may use at most 64 MiB of HBM per device.

```python
import math
import jax
import jax.numpy as jnp
import numpy as np
from jax import lax

D = 2048
FF = 1024
TOK_DEV = 256
EXPERTS = 8
CAP = 128
TOKENS = 4096
N_GR = 2
N_FS = 8
N_TP = 2


def block_levels(stream_key, dims, pieces, least, top_value):
    loudness, own = 1.0, jax.random.fold_in(stream_key, 6)
    for dim, parts in pieces:
        draws = jnp.exp(jax.random.uniform(jax.random.fold_in(own, dim), (parts,), jnp.float32, least / len(pieces), top_value / len(pieces)))
        loudness = loudness * jnp.repeat(draws, dims[dim] // parts).reshape([-1 if axis == dim else 1 for axis in range(len(dims))])
    return loudness


def assign_block(own_key, own, number, rows, count, top, most, slope):
    ranking = jax.random.permutation(own_key, count)
    crowded, usual = portions_of(count, rows * top, most, slope, True), portions_of(count, rows * top, most, slope, False)
    places = jnp.arange(count)

    def named(lengths, rotation):
        used = int((lengths > 0).sum())
        fixed = max(1, used // 4)
        moved = fixed + (places - fixed + rotation * (used - fixed)) % max(1, count - fixed)
        return jnp.zeros((count,), jnp.int32).at[ranking[jnp.where(places < fixed, places, moved)]].set(jnp.asarray(lengths, jnp.int32))

    lengths = jnp.where(number % 4 == 0, named(crowded, number // 4), named(usual, number - number // 4 - 1))
    mixed = jax.random.permutation(jax.random.fold_in(own, 3), count)
    source_of, receiver = mixed[0:count // 2 * 2:2], mixed[1:count // 2 * 2:2]
    slack = jnp.minimum(lengths[source_of] - 1, most - lengths[receiver]) // 2
    slack = jnp.where((source_of == ranking[0]) | (receiver == ranking[0]) | (lengths[receiver] == 0), 0, jnp.maximum(slack, 0))
    moved = jax.random.randint(jax.random.fold_in(own, 4), (count // 2,), 0, 1 << 20) % (slack + 1)
    lengths = lengths.at[source_of].add(-moved).at[receiver].add(moved)
    members = jnp.searchsorted(jnp.cumsum(lengths), jnp.arange(rows * top), side="right").astype(jnp.int32)
    table = members.reshape(top, rows).T
    table = table[jax.random.permutation(jax.random.fold_in(own, 1), rows)]
    rotation = jax.random.randint(jax.random.fold_in(own, 2), (rows, 1), 0, top)
    return jnp.take_along_axis(table, (jnp.arange(top)[None, :] + rotation) % top, axis=1)


def portions_of(amount, total, reach, slope, full):
    portions = [(1 << 20) // math.isqrt(standing ** slope) + 1 for standing in range(1, amount + 1)]
    largest = reach if full else min(reach, max(-(-total // amount), total * portions[0] // sum(portions)))
    least = 1 if total - largest >= amount - 1 else 0
    holding, rest = [largest] + [least] * (amount - 1), total - largest - least * (amount - 1)
    while rest > 0:
        candidates = [i for i in range(1, amount) if holding[i] < largest] or [i for i in range(1, amount) if holding[i] < reach]
        pool, left = sum([portions[i] for i in candidates]), rest
        for i in candidates:
            addition = min(reach - holding[i], max(1, left * portions[i] // pool), rest)
            holding[i] = holding[i] + addition
            rest = rest - addition
    return np.array(holding)


def gaussian(own_key, shape, scale, bound, split=(), kind=jnp.bfloat16):
    result = scale * jax.random.normal(own_key, shape, jnp.float32)
    if split:
        result = result * block_levels(own_key, shape, split, -0.22, 0.18)
    return jnp.clip(result, -bound, bound).astype(kind)


def setup_inputs(seed: int = 0) -> dict:
    key_list = jax.random.split(jax.random.key(seed), 8)
    tokens = gaussian(key_list[0], (TOKENS, D), 1.0, 6.0, ((0, 16),))
    norm_gain = jnp.clip(1.0 + 0.18 * jax.random.normal(key_list[1], (D,), jnp.float32), 0.1, 1.9)
    gate_train = gaussian(key_list[2], (EXPERTS, D, FF), D ** -0.5, 0.125, ((1, 16), (2, 2)), jnp.float32)
    up_train = gaussian(key_list[3], (EXPERTS, D, FF), D ** -0.5, 0.125, ((1, 16), (2, 2)), jnp.float32)
    down_train = gaussian(key_list[4], (EXPERTS, FF, D), FF ** -0.5, 0.1875, ((1, 2), (2, 16)), jnp.float32)
    expert_ids_keys = jax.random.split(jax.random.fold_in(key_list[5], 1), TOKENS // TOK_DEV)
    expert_ids_turns = jax.random.permutation(jax.random.fold_in(key_list[5], 3), TOKENS // TOK_DEV)
    expert_ids = jax.vmap(lambda own, number: assign_block(jax.random.fold_in(key_list[5], 2), own, number, TOK_DEV, EXPERTS, 2, CAP, 2))(expert_ids_keys, expert_ids_turns).reshape((TOKENS, 2))
    route_score = jnp.clip(jnp.exp(math.log(1.0) - 2.9957323 * jax.random.uniform(key_list[6], (TOKENS, 2), jnp.float32) ** block_levels(key_list[6], (TOKENS, 2), ((0, 16),), -0.2, 0.2)), 0.05, 1.0)
    return dict(tokens=tokens, norm_gain=norm_gain, gate_train=gate_train, up_train=up_train, down_train=down_train, expert_ids=expert_ids, route_score=route_score)


epsilon = 1e-06

def reference(tokens, norm_gain, gate_train, up_train, down_train, expert_ids, route_score):
    gate_ready = (norm_gain[None, :, None] * gate_train).astype(jnp.bfloat16)
    up_ready = (norm_gain[None, :, None] * up_train).astype(jnp.bfloat16)
    down_ready = down_train.astype(jnp.bfloat16)
    floated = tokens.astype(jnp.float32)
    normed = (floated * lax.rsqrt(lax.optimization_barrier(jnp.mean(floated * floated, axis=-1, keepdims=True)) + epsilon)).astype(jnp.bfloat16)
    route_share = route_score / lax.optimization_barrier(jnp.sum(route_score, axis=-1, keepdims=True))
    blocks = N_GR * N_FS
    picks = TOK_DEV * 2
    flat_ids = expert_ids.reshape(blocks, picks)
    flat_share = route_share.reshape(blocks, picks)
    token_of = ((jnp.arange(picks, dtype=jnp.int32) // 2)[None, :] + (jnp.arange(blocks, dtype=jnp.int32) * TOK_DEV)[:, None]).astype(jnp.int32)
    block_rows = jnp.broadcast_to(jnp.arange(blocks, dtype=jnp.int32)[:, None], (blocks, picks))
    hidden_block = FF // N_TP

    def per_expert(total, expert):
        matches = (flat_ids == expert).astype(jnp.int32)
        ranked = jnp.cumsum(matches, axis=1) - 1
        column = jnp.where(matches > 0, ranked, CAP).astype(jnp.int32)
        token_table = jnp.zeros((blocks, CAP), jnp.int32).at[block_rows, column].set(token_of, mode='drop')
        share_table = jnp.zeros((blocks, CAP), jnp.float32).at[block_rows, column].set(flat_share, mode='drop')
        token_index = token_table.reshape(-1)
        picked_rows = normed[token_index]
        gate_act = jnp.dot(picked_rows, gate_ready[expert], preferred_element_type=jnp.float32)
        up_act = jnp.dot(picked_rows, up_ready[expert], preferred_element_type=jnp.float32)
        hidden = (jax.nn.silu(gate_act) * up_act).astype(jnp.bfloat16)
        partial_value = jnp.einsum('rnh,nhk->rnk', hidden.reshape(-1, N_TP, hidden_block).astype(jnp.float32), down_ready[expert].reshape(N_TP, hidden_block, D).astype(jnp.float32))
        rounded = lax.optimization_barrier(partial_value.astype(jnp.bfloat16))
        expert_out = lax.optimization_barrier(jnp.sum(rounded.astype(jnp.float32), axis=1)).astype(jnp.bfloat16)
        total = total.at[token_index].add(share_table.reshape(-1)[:, None] * expert_out.astype(jnp.float32))
        return (total, None)
    start = jnp.zeros((TOKENS, D), jnp.float32)
    summed, _ = lax.scan(per_expert, start, jnp.arange(EXPERTS, dtype=jnp.int32))
    return (gate_ready, up_ready, down_ready, summed.astype(jnp.bfloat16))
```

```python
import jax
import jax.numpy as jnp
from jax import lax
from jax.sharding import PartitionSpec as P

epsilon = 1e-06


def shifted(value, name, step):
    count = lax.axis_size(name)
    return lax.ppermute(value, name, [(i, (i + step) % count) for i in range(count)])


def in_order(own, name):
    count = lax.axis_size(name)
    place = lax.axis_index(name)
    pieces = [own] + [shifted(own, name, step) for step in range(1, count)]
    if count == 1:
        return pieces
    if count == 2:
        return [jnp.where(place == j, pieces[0], pieces[1]) for j in range(2)]
    return [lax.select_n((place - j) % count, *pieces) for j in range(count)]


def on_device(tokens, norm_gain, gate_train, up_train, down_train, expert_ids, route_score):
    fs_count = lax.axis_size("fs")
    tp_count = lax.axis_size("tp")
    tp_place = lax.axis_index("tp")
    experts, rows, hidden_width = gate_train.shape
    tok_count, width = tokens.shape
    capacity = 4 * tok_count // experts
    served = experts // fs_count
    half = fs_count // 2
    half_experts = half * served
    part = width // tp_count

    gate_cast = (norm_gain[None, :, None] * gate_train).astype(jnp.bfloat16)
    up_cast = (norm_gain[None, :, None] * up_train).astype(jnp.bfloat16)
    down_cast = down_train.astype(jnp.bfloat16)
    both_cast = jnp.stack([gate_cast, up_cast], axis=1)
    both = lax.all_to_all(both_cast, "fs", split_axis=0, concat_axis=0, tiled=True)
    both = both.reshape(fs_count, served, 2, rows, hidden_width)

    floated = tokens.astype(jnp.float32)
    scale = lax.rsqrt(jnp.mean(floated * floated, axis=-1, keepdims=True) + epsilon)
    share = lax.dynamic_slice_in_dim(tokens, tp_place * part, part, axis=1)
    normed = (share.astype(jnp.float32) * scale).astype(jnp.bfloat16)
    flat_ids = expert_ids.reshape(-1)
    matches = (flat_ids[:, None] == jnp.arange(experts, dtype=jnp.int32)[None, :]).astype(jnp.int32)
    ranked = jnp.sum((jnp.cumsum(matches, axis=0) - 1) * matches, axis=1)
    slot_index = flat_ids * capacity + ranked
    pick_token = jnp.arange(flat_ids.shape[0], dtype=jnp.int32) // 2
    slot_token = jnp.zeros((experts * capacity,), jnp.int32).at[slot_index].set(pick_token)
    mirror_rows = shifted(normed, "fs", half)
    mirror_slots = shifted(slot_token, "fs", half)
    upper = lax.axis_index("fs") // half
    own_slots = lax.dynamic_slice_in_dim(
        slot_token.reshape(2, half_experts, capacity), upper, 1, axis=0
    )[0]
    far_slots = lax.dynamic_slice_in_dim(
        mirror_slots.reshape(2, half_experts, capacity), upper, 1, axis=0
    )[0] + tok_count
    first = jnp.where(upper == 0, own_slots, far_slots)
    second = jnp.where(upper == 0, far_slots, own_slots)
    pool = jnp.concatenate([normed, mirror_rows], axis=0)
    chosen = jnp.stack([first, second], axis=1).reshape(-1)
    outgoing = pool[chosen].reshape(half_experts, 2, capacity, part)

    down_cast, both = lax.optimization_barrier((down_cast, both))
    down = lax.all_to_all(down_cast, "fs", split_axis=0, concat_axis=0, tiled=True)
    down = down.reshape(fs_count, served, hidden_width, rows)
    outgoing, down = lax.optimization_barrier((outgoing, down))
    groups = [list(range(half)), list(range(half, 2 * half))]
    received = lax.all_to_all(
        outgoing, "fs", split_axis=0, concat_axis=0, tiled=True, axis_index_groups=groups
    )
    received = received.reshape(half, served, 2, capacity, part)
    by_expert = received.transpose(1, 0, 2, 3, 4).reshape(served, half * 2 * capacity, part)

    both_parts = in_order(both, "gr")
    gate_ready = jnp.concatenate(
        [p[:, :, 0].transpose(1, 0, 2, 3).reshape(served, -1, hidden_width) for p in both_parts], axis=1
    )
    up_ready = jnp.concatenate(
        [p[:, :, 1].transpose(1, 0, 2, 3).reshape(served, -1, hidden_width) for p in both_parts], axis=1
    )
    down_parts = in_order(down, "gr")
    down_ready = jnp.concatenate(
        [p.transpose(1, 2, 0, 3).reshape(served, hidden_width, -1) for p in down_parts], axis=2
    )

    gate_act = up_act = 0.0
    for step in range(tp_count):
        piece = shifted(by_expert, "tp", step) if step else by_expert
        start = ((tp_place - step) % tp_count) * part
        gate_piece = lax.dynamic_slice_in_dim(gate_ready, start, part, axis=1)
        up_piece = lax.dynamic_slice_in_dim(up_ready, start, part, axis=1)
        gate_act = gate_act + jnp.einsum(
            "enk,ekh->enh", piece, gate_piece, preferred_element_type=jnp.float32
        )
        up_act = up_act + jnp.einsum(
            "enk,ekh->enh", piece, up_piece, preferred_element_type=jnp.float32
        )
    hidden = (jax.nn.silu(gate_act) * up_act).astype(jnp.bfloat16)
    summed = 0.0
    for step in range(tp_count):
        start = ((tp_place + step) % tp_count) * part
        down_piece = lax.dynamic_slice_in_dim(down_ready, start, part, axis=2)
        value = jnp.einsum(
            "enh,ehk->enk", hidden, down_piece, preferred_element_type=jnp.float32
        ).astype(jnp.bfloat16)
        value = shifted(value, "tp", step) if step else value
        summed = summed + value.astype(jnp.float32)
    expert_out = summed.astype(jnp.bfloat16).reshape(served, half, 2, capacity, part)
    leaving = expert_out.transpose(2, 1, 0, 3, 4).reshape(experts, capacity, part)
    returned = lax.all_to_all(leaving, "fs", split_axis=0, concat_axis=0, tiled=True)
    flat_back = returned.reshape(experts * capacity, part)
    picked = flat_back[slot_index].reshape(tok_count, 2, part)
    route_share = route_score / jnp.sum(route_score, axis=-1, keepdims=True)
    mixed = jnp.sum(picked.astype(jnp.float32) * route_share[:, :, None], axis=1).astype(
        jnp.bfloat16
    )
    return (gate_ready, up_ready, down_ready, mixed)


def solution(mesh):
    return jax.shard_map(
        on_device,
        mesh=mesh,
        in_specs=(
            P(("gr", "fs"), None),
            P(("gr", "fs")),
            P(None, ("gr", "fs"), "tp"),
            P(None, ("gr", "fs"), "tp"),
            P(None, "tp", ("gr", "fs")),
            P(("gr", "fs"), None),
            P(("gr", "fs"), None),
        ),
        out_specs=(
            P("fs", None, "tp"),
            P("fs", None, "tp"),
            P("fs", "tp", None),
            P(("gr", "fs"), "tp"),
        ),
        check_vma=False,
    )
```

```python
import jax
import jax.numpy as jnp
from jax import lax
from jax.sharding import PartitionSpec as P

epsilon = 1e-06


def shifted(value, name, step):
    count = lax.axis_size(name)
    return lax.ppermute(value, name, [(i, (i + step) % count) for i in range(count)])


def in_order(own, name):
    count = lax.axis_size(name)
    place = lax.axis_index(name)
    pieces = [own] + [shifted(own, name, step) for step in range(1, count)]
    if count == 1:
        return pieces
    if count == 2:
        return [jnp.where(place == j, pieces[0], pieces[1]) for j in range(2)]
    return [lax.select_n((place - j) % count, *pieces) for j in range(count)]


def on_device(tokens, norm_gain, gate_train, up_train, down_train, expert_ids, route_score):
    fs_count = lax.axis_size("fs")
    tp_count = lax.axis_size("tp")
    tp_place = lax.axis_index("tp")
    experts, rows, hidden_width = gate_train.shape
    tok_count, width = tokens.shape
    capacity = 4 * tok_count // experts
    served = experts // fs_count
    half = fs_count // 2
    half_experts = half * served
    part = width // tp_count

    gate_cast = (norm_gain[None, :, None] * gate_train).astype(jnp.bfloat16)
    up_cast = (norm_gain[None, :, None] * up_train).astype(jnp.bfloat16)
    down_cast = down_train.astype(jnp.bfloat16)
    both_cast = jnp.stack([gate_cast, up_cast], axis=1)
    both = lax.all_to_all(both_cast, "fs", split_axis=0, concat_axis=0, tiled=True)
    both = both.reshape(fs_count, served, 2, rows, hidden_width)

    floated = tokens.astype(jnp.float32)
    scale = lax.rsqrt(jnp.mean(floated * floated, axis=-1, keepdims=True) + epsilon)
    share = lax.dynamic_slice_in_dim(tokens, tp_place * part, part, axis=1)
    normed = (share.astype(jnp.float32) * scale).astype(jnp.bfloat16)
    flat_ids = expert_ids.reshape(-1)
    matches = (flat_ids[:, None] == jnp.arange(experts, dtype=jnp.int32)[None, :]).astype(jnp.int32)
    ranked = jnp.sum((jnp.cumsum(matches, axis=0) - 1) * matches, axis=1)
    slot_index = flat_ids * capacity + ranked
    pick_token = jnp.arange(flat_ids.shape[0], dtype=jnp.int32) // 2
    slot_token = jnp.zeros((experts * capacity,), jnp.int32).at[slot_index].set(pick_token)
    mirror_rows = shifted(normed, "fs", half)
    mirror_slots = shifted(slot_token, "fs", half)
    upper = lax.axis_index("fs") // half

    def rows_for_half(pool, slots):
        mine = lax.dynamic_slice_in_dim(
            slots.reshape(2, half_experts * capacity), upper, 1, axis=0
        )[0]
        return pool[mine].reshape(half_experts, capacity, part)

    def over_half(outgoing):
        groups = [list(range(half)), list(range(half, 2 * half))]
        received = lax.all_to_all(
            outgoing, "fs", split_axis=0, concat_axis=0, tiled=True, axis_index_groups=groups
        )
        received = received.reshape(half, served, capacity, part)
        return received.transpose(1, 0, 2, 3).reshape(served, half * capacity, part)

    near_rows = rows_for_half(normed, slot_token)
    near_rows, both = lax.optimization_barrier((near_rows, both))
    near = over_half(near_rows)
    down_cast, near = lax.optimization_barrier((down_cast, near))
    down = lax.all_to_all(down_cast, "fs", split_axis=0, concat_axis=0, tiled=True)
    down = down.reshape(fs_count, served, hidden_width, rows)
    far_rows = rows_for_half(mirror_rows, mirror_slots)
    far_rows, down = lax.optimization_barrier((far_rows, down))
    far = over_half(far_rows)

    both_parts = in_order(both, "gr")
    gate_ready = jnp.concatenate(
        [p[:, :, 0].transpose(1, 0, 2, 3).reshape(served, -1, hidden_width) for p in both_parts], axis=1
    )
    up_ready = jnp.concatenate(
        [p[:, :, 1].transpose(1, 0, 2, 3).reshape(served, -1, hidden_width) for p in both_parts], axis=1
    )
    down_parts = in_order(down, "gr")
    down_ready = jnp.concatenate(
        [p.transpose(1, 2, 0, 3).reshape(served, hidden_width, -1) for p in down_parts], axis=2
    )

    def hidden_of(by_expert):
        gate_act = up_act = 0.0
        for step in range(tp_count):
            piece = shifted(by_expert, "tp", step) if step else by_expert
            start = ((tp_place - step) % tp_count) * part
            gate_piece = lax.dynamic_slice_in_dim(gate_ready, start, part, axis=1)
            up_piece = lax.dynamic_slice_in_dim(up_ready, start, part, axis=1)
            gate_act = gate_act + jnp.einsum(
                "enk,ekh->enh", piece, gate_piece, preferred_element_type=jnp.float32
            )
            up_act = up_act + jnp.einsum(
                "enk,ekh->enh", piece, up_piece, preferred_element_type=jnp.float32
            )
        return (jax.nn.silu(gate_act) * up_act).astype(jnp.bfloat16)

    near_hidden = hidden_of(near)
    far_hidden = hidden_of(far)
    hidden = jnp.concatenate(
        [
            jnp.where(upper == 0, near_hidden, far_hidden),
            jnp.where(upper == 0, far_hidden, near_hidden),
        ],
        axis=1,
    )
    summed = 0.0
    for step in range(tp_count):
        start = ((tp_place + step) % tp_count) * part
        down_piece = lax.dynamic_slice_in_dim(down_ready, start, part, axis=2)
        value = jnp.einsum(
            "enh,ehk->enk", hidden, down_piece, preferred_element_type=jnp.float32
        ).astype(jnp.bfloat16)
        value = shifted(value, "tp", step) if step else value
        summed = summed + value.astype(jnp.float32)
    expert_out = summed.astype(jnp.bfloat16).reshape(served, fs_count, capacity, part)
    leaving = expert_out.transpose(1, 0, 2, 3).reshape(experts, capacity, part)
    returned = lax.all_to_all(leaving, "fs", split_axis=0, concat_axis=0, tiled=True)
    flat_back = returned.reshape(experts * capacity, part)
    picked = flat_back[slot_index].reshape(tok_count, 2, part)
    route_share = route_score / jnp.sum(route_score, axis=-1, keepdims=True)
    mixed = jnp.sum(picked.astype(jnp.float32) * route_share[:, :, None], axis=1).astype(
        jnp.bfloat16
    )
    return (gate_ready, up_ready, down_ready, mixed)


def solution(mesh):
    return jax.shard_map(
        on_device,
        mesh=mesh,
        in_specs=(
            P(("gr", "fs"), None),
            P(("gr", "fs")),
            P(None, ("gr", "fs"), "tp"),
            P(None, ("gr", "fs"), "tp"),
            P(None, "tp", ("gr", "fs")),
            P(("gr", "fs"), None),
            P(("gr", "fs"), None),
        ),
        out_specs=(
            P("fs", None, "tp"),
            P("fs", None, "tp"),
            P("fs", "tp", None),
            P(("gr", "fs"), "tp"),
        ),
        check_vma=False,
    )
```

```python
import jax
import jax.numpy as jnp
from jax import lax
from jax.sharding import PartitionSpec as P

epsilon = 1e-06


def shifted(value, name, step):
    count = lax.axis_size(name)
    return lax.ppermute(value, name, [(i, (i + step) % count) for i in range(count)])


def in_order(own, name):
    count = lax.axis_size(name)
    place = lax.axis_index(name)
    pieces = [own] + [shifted(own, name, step) for step in range(1, count)]
    if count == 1:
        return pieces
    if count == 2:
        return [jnp.where(place == j, pieces[0], pieces[1]) for j in range(2)]
    return [lax.select_n((place - j) % count, *pieces) for j in range(count)]


def on_device(tokens, norm_gain, gate_train, up_train, down_train, expert_ids, route_score):
    fs_count = lax.axis_size("fs")
    tp_count = lax.axis_size("tp")
    tp_place = lax.axis_index("tp")
    experts, rows, hidden_width = gate_train.shape
    tok_count, width = tokens.shape
    capacity = 4 * tok_count // experts
    served = experts // fs_count
    half = fs_count // 2
    half_experts = half * served
    part = width // tp_count

    gate_cast = (norm_gain[None, :, None] * gate_train).astype(jnp.bfloat16)
    up_cast = (norm_gain[None, :, None] * up_train).astype(jnp.bfloat16)
    down_cast = down_train.astype(jnp.bfloat16)
    both_cast = jnp.stack([gate_cast, up_cast], axis=1)
    both = lax.all_to_all(both_cast, "fs", split_axis=0, concat_axis=0, tiled=True)
    both = both.reshape(fs_count, served, 2, rows, hidden_width)

    floated = tokens.astype(jnp.float32)
    scale = lax.rsqrt(jnp.mean(floated * floated, axis=-1, keepdims=True) + epsilon)
    share = lax.dynamic_slice_in_dim(tokens, tp_place * part, part, axis=1)
    normed = (share.astype(jnp.float32) * scale).astype(jnp.bfloat16)
    flat_ids = expert_ids.reshape(-1)
    matches = (flat_ids[:, None] == jnp.arange(experts, dtype=jnp.int32)[None, :]).astype(jnp.int32)
    ranked = jnp.sum((jnp.cumsum(matches, axis=0) - 1) * matches, axis=1)
    slot_index = flat_ids * capacity + ranked
    pick_token = jnp.arange(flat_ids.shape[0], dtype=jnp.int32) // 2
    slot_token = jnp.zeros((experts * capacity,), jnp.int32).at[slot_index].set(pick_token)
    mirror_rows = shifted(normed, "fs", half)
    mirror_slots = shifted(slot_token, "fs", half)
    upper = lax.axis_index("fs") // half
    own_slots = lax.dynamic_slice_in_dim(
        slot_token.reshape(2, half_experts, capacity), upper, 1, axis=0
    )[0]
    far_slots = lax.dynamic_slice_in_dim(
        mirror_slots.reshape(2, half_experts, capacity), upper, 1, axis=0
    )[0] + tok_count
    first = jnp.where(upper == 0, own_slots, far_slots)
    second = jnp.where(upper == 0, far_slots, own_slots)
    pool = jnp.concatenate([normed, mirror_rows], axis=0)
    chosen = jnp.stack([first, second], axis=1).reshape(-1)
    outgoing = pool[chosen].reshape(half_experts, 2, capacity, part)

    down_cast, both = lax.optimization_barrier((down_cast, both))
    down = lax.all_to_all(down_cast, "fs", split_axis=0, concat_axis=0, tiled=True)
    down = down.reshape(fs_count, served, hidden_width, rows)
    outgoing, down = lax.optimization_barrier((outgoing, down))
    groups = [list(range(half)), list(range(half, 2 * half))]
    received = lax.all_to_all(
        outgoing, "fs", split_axis=0, concat_axis=0, tiled=True, axis_index_groups=groups
    )
    received = received.reshape(half, served, 2, capacity, part)
    by_expert = received.transpose(1, 0, 2, 3, 4).reshape(served, half * 2 * capacity, part)

    both_parts = in_order(both, "gr")
    gate_ready = jnp.concatenate(
        [p[:, :, 0].transpose(1, 0, 2, 3).reshape(served, -1, hidden_width) for p in both_parts], axis=1
    )
    up_ready = jnp.concatenate(
        [p[:, :, 1].transpose(1, 0, 2, 3).reshape(served, -1, hidden_width) for p in both_parts], axis=1
    )
    down_parts = in_order(down, "gr")
    down_ready = jnp.concatenate(
        [p.transpose(1, 2, 0, 3).reshape(served, hidden_width, -1) for p in down_parts], axis=2
    )

    gate_act = up_act = 0.0
    for step in range(tp_count):
        piece = shifted(by_expert, "tp", step) if step else by_expert
        start = ((tp_place - step) % tp_count) * part
        gate_piece = lax.dynamic_slice_in_dim(gate_ready, start, part, axis=1)
        up_piece = lax.dynamic_slice_in_dim(up_ready, start, part, axis=1)
        gate_act = gate_act + jnp.einsum(
            "enk,ekh->enh", piece, gate_piece, preferred_element_type=jnp.float32
        )
        up_act = up_act + jnp.einsum(
            "enk,ekh->enh", piece, up_piece, preferred_element_type=jnp.float32
        )
    hidden = (jax.nn.silu(gate_act) * up_act).astype(jnp.bfloat16)
    summed = 0.0
    for step in range(tp_count):
        start = ((tp_place + step) % tp_count) * part
        down_piece = lax.dynamic_slice_in_dim(down_ready, start, part, axis=2)
        value = jnp.einsum(
            "enh,ehk->enk", hidden, down_piece, preferred_element_type=jnp.float32
        ).astype(jnp.bfloat16)
        value = shifted(value, "tp", step) if step else value
        summed = summed + value.astype(jnp.float32)
    expert_out = summed.astype(jnp.bfloat16).reshape(served, half, 2, capacity, part)
    leaving = expert_out.transpose(2, 1, 0, 3, 4).reshape(experts, capacity, part)
    returned = lax.all_to_all(leaving, "fs", split_axis=0, concat_axis=0, tiled=True)
    flat_back = returned.reshape(experts * capacity, part)
    route_share = route_score / jnp.sum(route_score, axis=-1, keepdims=True)
    pick_slots = slot_index.reshape(tok_count, 2)
    mixed = sum(
        flat_back[pick_slots[:, k]].astype(jnp.float32) * route_share[:, k, None] for k in range(2)
    ).astype(jnp.bfloat16)
    return (gate_ready, up_ready, down_ready, mixed)


def solution(mesh):
    return jax.shard_map(
        on_device,
        mesh=mesh,
        in_specs=(
            P(("gr", "fs"), None),
            P(("gr", "fs")),
            P(None, ("gr", "fs"), "tp"),
            P(None, ("gr", "fs"), "tp"),
            P(None, "tp", ("gr", "fs")),
            P(("gr", "fs"), None),
            P(("gr", "fs"), None),
        ),
        out_specs=(
            P("fs", None, "tp"),
            P("fs", None, "tp"),
            P("fs", "tp", None),
            P(("gr", "fs"), "tp"),
        ),
        check_vma=False,
    )
```
